32 devices in a mesh: ep: 8 (over z, x), tp: 4 (over y, core).
Axes of the slice: x: 2, y: 2, z: 4, core: 2. Of those that a mesh axis runs over, the one named last changes fastest.
Arguments:
- queries: bfloat16 [2048, 8, 128], P('ep', 'tp'), may hold values from -256 to 256
- keys: bfloat16 [2048, 4, 128], P('ep', 'tp'), may hold values from -8 to 8
- values: bfloat16 [2048, 4, 128], P('ep', 'tp'), may hold values from -6 to 6
- attn_lambda: float32 [8], P('tp'), may hold values from 0.3 to 0.8
- head_gain: float32 [128], replicated, may hold values from 0.1 to 1.9
- w_out: bfloat16 [1024, 2048], replicated, may hold values from -0.1875 to 0.1875
- moe_rows: bfloat16 [4096, 2048], P('ep'), may hold values from -6 to 6
- moe_gain: float32 [2048], replicated, may hold values from 0.1 to 1.9
- routes: int32 [4096, 2], P('ep'), may hold values from 0 to 7, all different within a row; in each aligned block of 128 rows (0 to 127, 128 to 255, ...) at most 64 rows name the same one
- route_weights: float32 [4096, 2], P('ep'), may hold values from 0.1 to 1
- w_gate: bfloat16 [8, 2048, 1024], P('ep', None, 'tp'), may hold values from -0.125 to 0.125
- w_up: bfloat16 [8, 2048, 1024], P('ep', None, 'tp'), may hold values from -0.125 to 0.125
- w_down: bfloat16 [8, 1024, 2048], P('ep', 'tp'), may hold values from -0.1875 to 0.1875
Outputs:
- mixer_out: bfloat16 [2048, 2048], P(('ep', 'tp'))
- moe_out: bfloat16 [4096, 2048], P(('ep', 'tp'))
The draws below stay inside these ranges and needn't reach their ends.
Inputs may be any that keep to these rules, and one draw needn't show every extreme that they name: `routes`: each row names 2 different experts. In each aligned block of 128 rows (the rows of moe_out that one device holds) no expert is named by more than 64 rows, a bound that some block reaches.
All inputs are finite; a program needn't handle non-finite values.
Results may differ from the reference program's by a relative error of at most 0.011.
Values may be sent and summed in bfloat16 or wider, within the bound.
A program may use at most 128 MiB of HBM per device.

```python
import math
import jax
import jax.numpy as jnp
import numpy as np
from jax import lax

D = 2048
HQ = 8
KVH = 4
HEAD = 64
VDIM = 128
FF = 1024
TOPK = 2
MOE_DEV = 128
EXPERTS = 8
CAP = 64
ATT_TOKENS = 2048
MOE_TOKENS = 4096
N_EP = 8
N_TP = 4


def pair_draw(key):
    spread = 1.75 ** 0.5
    base_q = jax.random.truncated_normal(jax.random.fold_in(key, 101), -4.5, 4.5, (ATT_TOKENS, HQ, 2, HEAD), jnp.float32) * spread
    base_k = jax.random.truncated_normal(jax.random.fold_in(key, 102), -4.5, 4.5, (ATT_TOKENS, KVH, 2, HEAD), jnp.float32) * spread
    return (base_q.reshape(ATT_TOKENS, HQ, 2 * HEAD), base_k.reshape(ATT_TOKENS, KVH, 2 * HEAD))


def draw_queries(key, part):
    return pair_draw(key)[0].astype(jnp.bfloat16)


def draw_keys(key, part):
    return pair_draw(key)[1].astype(jnp.bfloat16)


def steps_of(key, shape, shards, low, high):
    factor_of = 1.0
    for dim, blocks in shards:
        steps = jax.random.uniform(jax.random.fold_in(jax.random.fold_in(key, 6), dim), (blocks,), jnp.float32, low / len(shards), high / len(shards))
        factor_of = factor_of * jnp.repeat(jnp.exp(steps), shape[dim] // blocks).reshape((-1,) + (1,) * (len(shape) - 1 - dim))
    return factor_of


def deal_out(key, own, number, rows, number_of, top, limit, slope):
    order = jax.random.permutation(key, number_of)
    heavy_load, ordinary = load_shares(number_of, rows * top, limit, slope, True), load_shares(number_of, rows * top, limit, slope, False)
    places = jnp.arange(number_of)

    def named(tallies, offset_by):
        used = int((tallies > 0).sum())
        fixed = max(1, used // 4)
        moved = fixed + (places - fixed + offset_by * (used - fixed)) % max(1, number_of - fixed)
        return jnp.zeros((number_of,), jnp.int32).at[order[jnp.where(places < fixed, places, moved)]].set(jnp.asarray(tallies, jnp.int32))

    tallies = jnp.where(number % 4 == 0, named(heavy_load, number // 4), named(ordinary, number - number // 4 - 1))
    mixed = jax.random.permutation(jax.random.fold_in(own, 3), number_of)
    source_of, taker = mixed[0:number_of // 2 * 2:2], mixed[1:number_of // 2 * 2:2]
    slack = jnp.minimum(tallies[source_of] - 1, limit - tallies[taker]) // 2
    slack = jnp.where((source_of == order[0]) | (taker == order[0]) | (tallies[taker] == 0), 0, jnp.maximum(slack, 0))
    moved = jax.random.randint(jax.random.fold_in(own, 4), (number_of // 2,), 0, 1 << 20) % (slack + 1)
    tallies = tallies.at[source_of].add(-moved).at[taker].add(moved)
    members = jnp.searchsorted(jnp.cumsum(tallies), jnp.arange(rows * top), side="right").astype(jnp.int32)
    table = members.reshape(top, rows).T
    table = table[jax.random.permutation(jax.random.fold_in(own, 1), rows)]
    offset_by = jax.random.randint(jax.random.fold_in(own, 2), (rows, 1), 0, top)
    return jnp.take_along_axis(table, (jnp.arange(top)[None, :] + offset_by) % top, axis=1)


def load_shares(amount, total, bound, lean, full):
    weights = [(1 << 20) // math.isqrt(standing ** lean) + 1 for standing in range(1, amount + 1)]
    largest = bound if full else min(bound, max(-(-total // amount), total * weights[0] // sum(weights)))
    least = 1 if total - largest >= amount - 1 else 0
    counts, spare = [largest] + [least] * (amount - 1), total - largest - least * (amount - 1)
    while spare > 0:
        free = [i for i in range(1, amount) if counts[i] < largest] or [i for i in range(1, amount) if counts[i] < bound]
        pool, budget = sum([weights[i] for i in free]), spare
        for i in free:
            extra = min(bound - counts[i], max(1, budget * weights[i] // pool), spare)
            counts[i] = counts[i] + extra
            spare = spare - extra
    return np.array(counts)


def normal_values(rng, extent, deviation, limit, split=(), kind=jnp.bfloat16):
    entries = deviation * jax.random.normal(rng, extent, jnp.float32)
    if split:
        entries = entries * steps_of(rng, extent, split, -0.22, 0.18)
    return jnp.clip(entries, -limit, limit).astype(kind)


def setup_inputs(seed: int = 0) -> dict:
    streams_of = jax.random.split(jax.random.key(seed), 14)
    queries = draw_queries(jax.random.fold_in(streams_of[13], 71), 0)
    keys = draw_keys(jax.random.fold_in(streams_of[13], 71), 0)
    values = normal_values(streams_of[2], (ATT_TOKENS, KVH, VDIM), 1.0, 6.0, ((0, 8), (1, 4)))
    attn_lambda = jnp.clip(0.3 + 0.5 * jax.random.uniform(streams_of[3], (HQ,), jnp.float32) ** steps_of(streams_of[3], (HQ,), ((0, 4),), -0.2, 0.2), 0.3, 0.8)
    head_gain = jnp.clip(1.0 + 0.18 * jax.random.normal(streams_of[4], (VDIM,), jnp.float32), 0.1, 1.9)
    w_out = normal_values(streams_of[5], (HQ * VDIM, D), (HQ * VDIM) ** -0.5, 0.1875)
    moe_rows = normal_values(streams_of[6], (MOE_TOKENS, D), 1.0, 6.0, ((0, 8),))
    moe_gain = jnp.clip(1.0 + 0.18 * jax.random.normal(streams_of[7], (D,), jnp.float32), 0.1, 1.9)
    routes_keys = jax.random.split(jax.random.fold_in(streams_of[8], 1), MOE_TOKENS // MOE_DEV)
    routes_turns = jax.random.permutation(jax.random.fold_in(streams_of[8], 3), MOE_TOKENS // MOE_DEV)
    routes = jax.vmap(lambda own, number: deal_out(jax.random.fold_in(streams_of[8], 2), own, number, MOE_DEV, EXPERTS, TOPK, CAP, 1))(routes_keys, routes_turns).reshape((MOE_TOKENS, TOPK))
    route_weights = jnp.clip(0.1 + 0.9 * jax.random.uniform(streams_of[9], (MOE_TOKENS, TOPK), jnp.float32) ** steps_of(streams_of[9], (MOE_TOKENS, TOPK), ((0, 8),), -0.2, 0.2), 0.1, 1.0)
    w_gate = normal_values(streams_of[10], (EXPERTS, D, FF), D ** -0.5, 0.125, ((0, 8), (2, 4)))
    w_up = normal_values(streams_of[11], (EXPERTS, D, FF), D ** -0.5, 0.125, ((0, 8), (2, 4)))
    w_down = normal_values(streams_of[12], (EXPERTS, FF, D), FF ** -0.5, 0.1875, ((0, 8), (1, 4)))
    return dict(queries=queries, keys=keys, values=values, attn_lambda=attn_lambda, head_gain=head_gain, w_out=w_out, moe_rows=moe_rows, moe_gain=moe_gain, routes=routes, route_weights=route_weights, w_gate=w_gate, w_up=w_up, w_down=w_down)


EPSILON = 1e-06
MASKED = -1e+30

def reference(queries, keys, values, attn_lambda, head_gain, w_out, moe_rows, moe_gain, routes, route_weights, w_gate, w_up, w_down):
    length = queries.shape[0]
    per_key = HQ // KVH
    key_all = jnp.repeat(keys.astype(jnp.float32).reshape(length, KVH, 2, HEAD), per_key, axis=1)
    value_all = jnp.repeat(values.astype(jnp.float32), per_key, axis=1)
    block_len = math.gcd(length, 256)
    block_count = length // block_len
    query_all = queries.astype(jnp.float32).reshape(block_count, block_len, HQ, 2, HEAD)
    key_pos = jnp.arange(length, dtype=jnp.int32)

    def one_block(inputs):
        query_blk, block_index = inputs
        query_pos = block_index * block_len + jnp.arange(block_len, dtype=jnp.int32)
        scores = jnp.einsum('qhmd,khmd->hmqk', query_blk, key_all) * HEAD ** (-0.5)
        allowed = key_pos[None, :] <= query_pos[:, None]
        scores = jnp.where(allowed, scores, MASKED)
        row_max = lax.optimization_barrier(jnp.max(scores, axis=-1, keepdims=True))
        weights = jnp.exp(scores - row_max)
        totals = lax.optimization_barrier(jnp.sum(weights, axis=-1))
        rounded = lax.optimization_barrier(weights.astype(jnp.bfloat16)).astype(jnp.float32)
        numerator = jnp.einsum('hmqk,khv->hmqv', rounded, value_all)
        ratios = numerator / totals[..., None]
        head_out = ratios[:, 0] - attn_lambda[:, None, None] * ratios[:, 1]
        inv_rms = lax.rsqrt(lax.optimization_barrier(jnp.mean(head_out * head_out, axis=-1, keepdims=True)) + EPSILON)
        normed_heads = (head_out * inv_rms * head_gain).astype(jnp.bfloat16)
        return jnp.transpose(normed_heads, (1, 0, 2)).reshape(block_len, HQ * VDIM)
    attn_rows = lax.map(one_block, (query_all, jnp.arange(block_count, dtype=jnp.int32)))
    attn_rows = attn_rows.reshape(length, HQ * VDIM)
    mixer_out = jnp.dot(attn_rows, w_out, preferred_element_type=jnp.float32).astype(jnp.bfloat16)
    rows_f = moe_rows.astype(jnp.float32)
    normed = (rows_f * lax.rsqrt(lax.optimization_barrier(jnp.mean(rows_f * rows_f, axis=-1, keepdims=True)) + EPSILON) * moe_gain).astype(jnp.bfloat16)
    tokens = moe_rows.shape[0]
    pairs = tokens * TOPK
    flat_ids = routes.reshape(-1).astype(jnp.int32)
    matches = (flat_ids[:, None] == jnp.arange(EXPERTS, dtype=jnp.int32)[None, :]).astype(jnp.int32)
    earlier = jnp.cumsum(matches, axis=0) - matches
    position = lax.optimization_barrier(jnp.sum(earlier * matches, axis=1)).astype(jnp.int32)
    slot_total = N_EP * N_TP * CAP
    pair_table = jnp.full((EXPERTS, slot_total), pairs, dtype=jnp.int32)
    pair_table = pair_table.at[flat_ids, position].set(jnp.arange(pairs, dtype=jnp.int32))
    token_table = jnp.where(pair_table < pairs, pair_table // TOPK, tokens).astype(jnp.int32)
    weight_flat = jnp.concatenate([route_weights.reshape(-1), jnp.zeros((1,), jnp.float32)])
    weight_table = weight_flat[pair_table]
    padded = jnp.concatenate([normed, jnp.zeros((1, D), jnp.bfloat16)], axis=0)
    group_width = FF // N_TP

    def one_expert(accumulated, inputs):
        token_row, weight_row, gate_w, up_w, down_w = inputs
        chosen = padded[token_row]
        gate_out = jnp.dot(chosen, gate_w, preferred_element_type=jnp.float32)
        up_out = jnp.dot(chosen, up_w, preferred_element_type=jnp.float32)
        hidden = (jax.nn.silu(gate_out) * up_out).astype(jnp.bfloat16)
        partials = jnp.einsum('stf,tfd->tsd', hidden.reshape(slot_total, N_TP, group_width).astype(jnp.float32), down_w.reshape(N_TP, group_width, D).astype(jnp.float32))
        partials = lax.optimization_barrier(partials.astype(jnp.bfloat16)).astype(jnp.float32)
        expert_out = lax.optimization_barrier(lax.optimization_barrier(jnp.sum(partials, axis=0)).astype(jnp.bfloat16)).astype(jnp.float32)
        accumulated = accumulated.at[token_row].add(weight_row[:, None] * expert_out)
        return (accumulated, None)
    start_total = jnp.zeros((tokens + 1, D), jnp.float32)
    accumulated, unused = lax.scan(one_expert, start_total, (token_table, weight_table, w_gate, w_up, w_down))
    moe_out = accumulated[:tokens].astype(jnp.bfloat16)
    return (mixer_out, moe_out)
```

```python
import functools

import jax
import jax.numpy as jnp
from jax import lax
from jax.experimental import pallas as pl
from jax.experimental.pallas import tpu as pltpu
from jax.sharding import PartitionSpec as P

EPSILON = 1e-06
MASKED = -1e30


def rms_scaled(values_f, gain):
    mean_sq = jnp.mean(values_f * values_f, axis=-1, keepdims=True)
    return values_f * lax.rsqrt(mean_sq + EPSILON) * gain


def expert_kernel(
    n,
    out_ref,
    mine_ref,
    gate_ref,
    up_ref,
    down_ref,
    mix_ref,
    res_ref,
    slots,
    part,
    pair_in,
    col_in,
    back,
    hidden_ref,
    acc,
    send_a,
    recv_a,
    send_y,
    recv_y,
    send_c,
    recv_c,
    send_b,
    recv_b,
    send_p,
    recv_p,
    send_q,
    recv_q,
    send_r,
    recv_r,
    local_sem,
):
    me = lax.axis_index("ep")
    tp = lax.axis_index("tp")
    row = tp // 2
    col = tp % 2
    other_row = 1 - row
    other_col = 1 - col
    pair_peer = row * 2 + other_col
    row_peer = other_row * 2 + col
    own_blk = col * 2 + row
    far_blk = col * 2 + other_row
    slot_count = slots.shape[2]
    width = slots.shape[3]

    def remote(src, dst, ssem, rsem, ep_id, tp_id):
        return pltpu.make_async_remote_copy(
            src_ref=src,
            dst_ref=dst,
            send_sem=ssem,
            recv_sem=rsem,
            device_id=(ep_id, tp_id),
            device_id_type=pl.DeviceIdType.MESH,
        )

    barrier = pltpu.get_barrier_semaphore()

    @pl.loop(1, n)
    def _(d):
        pl.semaphore_signal(
            barrier, inc=1, device_id=((me + d) % n, tp), device_id_type=pl.DeviceIdType.MESH
        )

    for peer in (pair_peer, row_peer):
        pl.semaphore_signal(
            barrier, inc=1, device_id=(me, peer), device_id_type=pl.DeviceIdType.MESH
        )
    fills = [
        pltpu.make_async_copy(
            mine_ref.at[b], slots.at[0, (b % 2) * 2 + b // 2], local_sem.at[b]
        )
        for b in range(4)
    ]
    for fill in fills:
        fill.start()
    pl.semaphore_wait(barrier, n + 1)

    def copy_a(d):
        return remote(
            out_ref.at[d], slots.at[d, own_blk], send_a.at[d], recv_a.at[d], (me + d) % n, tp
        )

    def copy_y(d):
        block = slots.at[d, own_blk]
        return remote(block, block, send_y.at[d], recv_y.at[d], me, row_peer)

    def copy_c(d):
        block = slots.at[d, own_blk]
        return remote(block, block, send_c.at[d], recv_c.at[d], me, pair_peer)

    def copy_b(d):
        block = slots.at[d, far_blk]
        return remote(block, block, send_b.at[d], recv_b.at[d], me, pair_peer)

    def copy_p(d):
        return remote(
            part.at[d, pl.ds(other_col * 2, 2)],
            pair_in.at[d],
            send_p.at[d],
            recv_p.at[d],
            me,
            pair_peer,
        )

    def copy_q(d):
        return remote(part.at[d, far_blk], col_in.at[d], send_q.at[d], recv_q.at[d], me, row_peer)

    def copy_r(d):
        return remote(
            part.at[d, own_blk], back.at[d], send_r.at[d], recv_r.at[d], (me + n - d) % n, tp
        )

    @pl.loop(1, n)
    def _(d):
        copy_a(d).start()

    for fill in fills:
        fill.wait()

    def merge(index, other):
        rows = part.at[index]
        step = min(512, width)

        @pl.loop(0, width // step)
        def _(c):
            cols = pl.ds(pl.multiple_of(c * step, step), step)
            rows[:, cols] = (
                rows[:, cols].astype(jnp.float32) + other[:, cols].astype(jnp.float32)
            ).astype(part.dtype)

    def one_block(rows, put):
        gate = jnp.dot(rows, gate_ref[...], preferred_element_type=jnp.float32)
        up = jnp.dot(rows, up_ref[...], preferred_element_type=jnp.float32)
        hidden_ref[...] = (gate / (1.0 + jnp.exp(-gate)) * up).astype(hidden_ref.dtype)
        step = min(512, width)

        @pl.loop(0, width // step)
        def _(c):
            cols = pl.ds(pl.multiple_of(c * step, step), step)
            put(
                cols,
                jnp.dot(
                    hidden_ref[...], down_ref[:, cols], preferred_element_type=jnp.float32
                ).astype(part.dtype),
            )

    def compute(j):
        if slot_count % 16 == 0:

            def put(cols, val):
                part[j, :, :, cols] = val.reshape(4, slot_count, val.shape[1])

            one_block(slots[j].reshape(4 * slot_count, width), put)
        else:

            @pl.loop(0, 4)
            def _(b):
                def put(cols, val):
                    part[j, b, :, cols] = val

                one_block(slots[j, b], put)

    def inside(j, low):
        return jnp.logical_and(j >= low, j < n)

    @pl.loop(0, n + 5)
    def _(i):
        @pl.when(inside(i, 1))
        def _():
            copy_a(i).wait_recv()
            copy_y(i).start()
            copy_c(i).start()

        @pl.when(inside(i - 1, 1))
        def _():
            copy_y(i - 1).wait_recv()
            copy_b(i - 1).start()

        @pl.when(inside(i - 5, 0))
        def _():
            copy_q(i - 5).wait_recv()
            merge((i - 5, own_blk), col_in.at[i - 5])

        @pl.when(inside(i - 3, 0))
        def _():
            copy_p(i - 3).wait_recv()
            for y in range(2):
                merge((i - 3, col * 2 + y), pair_in.at[i - 3, y])

        @pl.when(inside(i - 2, 1))
        def _():
            copy_c(i - 2).wait_recv()
            copy_b(i - 2).wait_recv()

        @pl.when(inside(i - 2, 0))
        def _():
            compute(i - 2)

        @pl.when(inside(i - 5, 1))
        def _():
            copy_r(i - 5).start()

        @pl.when(inside(i - 3, 0))
        def _():
            copy_q(i - 3).start()

        @pl.when(inside(i - 2, 0))
        def _():
            copy_p(i - 2).start()

    def collect(d, rows):
        mix = mix_ref[d]
        high = mix.astype(jnp.bfloat16)
        low = (mix - high.astype(jnp.float32)).astype(jnp.bfloat16)
        both = jnp.dot(high, rows, preferred_element_type=jnp.float32) + jnp.dot(
            low, rows, preferred_element_type=jnp.float32
        )
        return both

    acc[...] = collect(0, part[0, own_blk])

    @pl.loop(1, n)
    def _(d):
        copy_r(d).wait_recv()
        acc[...] += collect(d, back[d])

    res_ref[...] = acc[...].astype(res_ref.dtype)

    @pl.loop(1, n)
    def _(d):
        copy_a(d).wait_send()
        copy_y(d).wait_send()
        copy_c(d).wait_send()
        copy_b(d).wait_send()
        copy_r(d).wait_send()

    @pl.loop(0, n)
    def _(d):
        copy_p(d).wait_send()
        copy_q(d).wait_send()


def run_experts(outgoing, mine, gate_w, up_w, down_w, mix):
    n, capacity, width = outgoing.shape
    hidden_units = gate_w.shape[1]
    tokens = mix.shape[1]
    rows = 4 * capacity if capacity % 16 == 0 else capacity
    dtype = outgoing.dtype
    vmem = pl.BlockSpec(memory_space=pltpu.VMEM)
    flops = 2 * n * 4 * capacity * width * hidden_units * 3
    return pl.pallas_call(
        functools.partial(expert_kernel, n),
        out_shape=jax.ShapeDtypeStruct((tokens, width), dtype),
        in_specs=[vmem] * 6,
        out_specs=vmem,
        scratch_shapes=[
            pltpu.VMEM((n, 4, capacity, width), dtype),
            pltpu.VMEM((n, 4, capacity, width), dtype),
            pltpu.VMEM((n, 2, capacity, width), dtype),
            pltpu.VMEM((n, capacity, width), dtype),
            pltpu.VMEM((n, capacity, width), dtype),
            pltpu.VMEM((rows, hidden_units), dtype),
            pltpu.VMEM((tokens, width), jnp.float32),
        ]
        + [pltpu.SemaphoreType.DMA((n,))] * 14
        + [pltpu.SemaphoreType.DMA((4,))],
        compiler_params=pltpu.CompilerParams(
            collective_id=0, has_side_effects=True, vmem_limit_bytes=60 * 1024 * 1024
        ),
        cost_estimate=pl.CostEstimate(
            flops=40 * flops, bytes_accessed=16 * 1024 * 1024, transcendentals=0
        ),
    )(outgoing, mine, gate_w, up_w, down_w, mix)


def expert_part(moe_rows, moe_gain, routes, route_weights, w_gate, w_up, w_down):
    experts = lax.axis_size("ep")
    tp_count = lax.axis_size("tp")
    me = lax.axis_index("ep")
    tp_id = lax.axis_index("tp")
    dev_rows = moe_rows.shape[0] // tp_count
    top_count = routes.shape[1]
    capacity = max(2, 2 * dev_rows * top_count // experts)
    width = moe_rows.shape[1]
    normed = (
        rms_scaled(moe_rows.astype(jnp.float32), moe_gain)
        .astype(jnp.bfloat16)
        .reshape(tp_count, dev_rows, width)
    )
    relative = ((routes - me) % experts).reshape(tp_count, dev_rows, top_count)
    hits = relative[..., None] == lax.iota(jnp.int32, experts)
    named = jnp.any(hits, axis=2)
    before = (
        lax.iota(jnp.int32, dev_rows)[:, None] > lax.iota(jnp.int32, dev_rows)[None, :]
    ).astype(jnp.bfloat16)
    places = jnp.einsum(
        "ij,bjd->bid", before, named.astype(jnp.bfloat16), preferred_element_type=jnp.float32
    ).astype(jnp.int32)
    places = jnp.where(named, places, -1)
    slot_iota = lax.iota(jnp.int32, capacity)
    take_mine = (places[:, None, :, 0] == slot_iota[None, :, None]).astype(jnp.bfloat16)
    mine = jnp.einsum(
        "bst,btm->bsm", take_mine, normed, preferred_element_type=jnp.float32
    ).astype(jnp.bfloat16)
    own = lambda arr: lax.dynamic_index_in_dim(arr, tp_id, 0, keepdims=False)
    own_places = own(places)
    own_rows = own(normed)
    take = (own_places.T[:, None, :] == slot_iota[None, :, None]).astype(jnp.bfloat16)
    outgoing = (
        jnp.dot(
            take.reshape(experts * capacity, dev_rows),
            own_rows,
            preferred_element_type=jnp.float32,
        )
        .astype(jnp.bfloat16)
        .reshape(experts, capacity, width)
    )
    own_weights = own(route_weights.reshape(tp_count, dev_rows, top_count))
    weight_of = jnp.sum(jnp.where(own(hits), own_weights[..., None], 0.0), axis=1)
    mix = jnp.where(
        own_places.T[:, :, None] == slot_iota[None, None, :], weight_of.T[:, :, None], 0.0
    )
    return run_experts(outgoing, mine, w_gate[0], w_up[0], w_down[0], mix)


def local(
    queries,
    keys,
    values,
    attn_lambda,
    head_gain,
    w_out,
    moe_rows,
    moe_gain,
    routes,
    route_weights,
    w_gate,
    w_up,
    w_down,
):
    positions = queries.shape[0]
    q_heads = queries.shape[1]
    kv_heads = keys.shape[1]
    head_dim = queries.shape[2] // 2
    value_dim = values.shape[2]
    per_key = q_heads // kv_heads
    first_pos = lax.axis_index("ep") * positions
    query_pos = first_pos + lax.iota(jnp.int32, positions)
    last_pos = first_pos + positions - 1
    query_view = queries.reshape(positions, kv_heads, per_key, 2, head_dim)
    inv_scale = head_dim ** (-0.5)
    start_max = jnp.full((positions, kv_heads, per_key, 2), MASKED, jnp.float32)
    start_total = jnp.zeros((positions, kv_heads, per_key, 2), jnp.float32)
    start_acc = jnp.zeros((positions, kv_heads, per_key, 2, value_dim), jnp.float32)
    carry = (start_max, start_total, start_acc)
    both = jnp.concatenate([keys, values], axis=2)
    gathered = lax.all_gather(both, "ep", axis=0, tiled=True)
    key_piece = gathered[:, :, : keys.shape[2]]
    value_piece = gathered[:, :, keys.shape[2] :]
    shard_count = key_piece.shape[0] // positions
    together = 1
    for candidate in (2, 3, 4):
        if shard_count % candidate == 0:
            together = candidate
    block_len = together * positions
    blocks = shard_count // together
    key_blocks = key_piece.reshape(blocks, block_len, kv_heads, 2, head_dim)
    value_blocks = value_piece.reshape(blocks, block_len, kv_heads, value_dim)
    block_starts = block_len * lax.iota(jnp.int32, blocks)

    def visit(running, inputs):
        key_blk, value_blk, block_start = inputs

        def update(current):
            run_max, run_total, run_acc = current
            key_pos = block_start + lax.iota(jnp.int32, block_len)
            scores = (
                jnp.einsum(
                    "qkgmd,pkmd->qkgmp", query_view, key_blk, preferred_element_type=jnp.float32
                )
                * inv_scale
            )
            allowed = key_pos[None, :] <= query_pos[:, None]
            scores = jnp.where(allowed[:, None, None, None, :], scores, MASKED)
            new_max = jnp.maximum(run_max, jnp.max(scores, axis=-1))
            shrink = jnp.exp(run_max - new_max)
            weights = jnp.exp(scores - new_max[..., None])
            run_total = run_total * shrink + jnp.sum(weights, axis=-1)
            run_acc = run_acc * shrink[..., None] + jnp.einsum(
                "qkgmp,pkv->qkgmv",
                weights.astype(jnp.bfloat16),
                value_blk,
                preferred_element_type=jnp.float32,
            )
            return (new_max, run_total, run_acc)

        def keep(current):
            return current

        return (lax.cond(block_start <= last_pos, update, keep, running), None)

    carry, unused = lax.scan(visit, carry, (key_blocks, value_blocks, block_starts))
    run_max, run_total, run_acc = carry
    ratios = run_acc / run_total[..., None]
    lambda_view = attn_lambda.reshape(1, kv_heads, per_key, 1)
    head_out = ratios[:, :, :, 0] - lambda_view * ratios[:, :, :, 1]
    attn_rows = (
        rms_scaled(head_out, head_gain).astype(jnp.bfloat16).reshape(positions, q_heads * value_dim)
    )
    tp_count = lax.axis_size("tp")
    tp_id = lax.axis_index("tp")
    exchanged = lax.all_to_all(
        attn_rows.reshape(positions, q_heads, value_dim),
        "tp",
        split_axis=0,
        concat_axis=1,
        tiled=True,
    )
    mixer_out = jnp.dot(
        exchanged.reshape(positions // tp_count, tp_count * q_heads * value_dim),
        w_out,
        preferred_element_type=jnp.float32,
    ).astype(jnp.bfloat16)
    moe_out = expert_part(moe_rows, moe_gain, routes, route_weights, w_gate, w_up, w_down)
    return (mixer_out, moe_out)


def solution(mesh):
    return jax.shard_map(
        local,
        mesh=mesh,
        in_specs=(
            P("ep", "tp", None),
            P("ep", "tp", None),
            P("ep", "tp", None),
            P("tp"),
            P(),
            P(),
            P("ep", None),
            P(),
            P("ep", None),
            P("ep", None),
            P("ep", None, "tp"),
            P("ep", None, "tp"),
            P("ep", "tp", None),
        ),
        out_specs=(P(("ep", "tp"), None), P(("ep", "tp"), None)),
        check_vma=False,
    )
```

```python
import functools

import jax
import jax.numpy as jnp
from jax import lax
from jax.experimental import pallas as pl
from jax.experimental.pallas import tpu as pltpu
from jax.sharding import PartitionSpec as P

EPSILON = 1e-06
MASKED = -1e30


def rms_scaled(values_f, gain):
    mean_sq = jnp.mean(values_f * values_f, axis=-1, keepdims=True)
    return values_f * lax.rsqrt(mean_sq + EPSILON) * gain


def expert_kernel(
    n,
    out_ref,
    near_ref,
    mine_ref,
    gate_ref,
    up_ref,
    down_ref,
    mix_ref,
    res_ref,
    slots,
    part,
    pair_in,
    col_in,
    back,
    hidden_ref,
    acc,
    send_a,
    recv_a,
    send_y,
    recv_y,
    send_c,
    recv_c,
    send_b,
    recv_b,
    send_p,
    recv_p,
    send_q,
    recv_q,
    send_r,
    recv_r,
    local_sem,
):
    me = lax.axis_index("ep")
    tp = lax.axis_index("tp")
    row = tp // 2
    col = tp % 2
    other_row = 1 - row
    other_col = 1 - col
    pair_peer = row * 2 + other_col
    row_peer = other_row * 2 + col
    own_blk = col * 2 + row
    far_blk = col * 2 + other_row
    slot_count = slots.shape[2]
    width = slots.shape[3]

    near = near_ref.shape[0]
    bits = [1 << b for b in range(n.bit_length() - 1)]

    def partner(d):
        total = 0
        for bit in bits:
            total = total + (me // bit + d // bit) % 2 * bit
        return total

    def remote(src, dst, ssem, rsem, ep_id, tp_id):
        return pltpu.make_async_remote_copy(
            src_ref=src,
            dst_ref=dst,
            send_sem=ssem,
            recv_sem=rsem,
            device_id=(ep_id, tp_id),
            device_id_type=pl.DeviceIdType.MESH,
        )

    barrier = pltpu.get_barrier_semaphore()

    @pl.loop(1, n)
    def _(d):
        pl.semaphore_signal(
            barrier, inc=1, device_id=(partner(d), tp), device_id_type=pl.DeviceIdType.MESH
        )

    for peer in (pair_peer, row_peer):
        pl.semaphore_signal(
            barrier, inc=1, device_id=(me, peer), device_id_type=pl.DeviceIdType.MESH
        )
    fills = [
        pltpu.make_async_copy(
            mine_ref.at[b], slots.at[0, (b % 2) * 2 + b // 2], local_sem.at[b]
        )
        for b in range(4)
    ]
    for fill in fills:
        fill.start()
    pl.semaphore_wait(barrier, n + 1)

    def copy_a(d):
        return remote(
            out_ref.at[d], slots.at[d, own_blk], send_a.at[d], recv_a.at[d], partner(d), tp
        )

    def copy_n(d):
        return remote(
            near_ref.at[d], slots.at[d, far_blk], send_y.at[d], recv_y.at[d], partner(d), tp
        )

    def copy_y(d):
        block = slots.at[d, own_blk]
        return remote(block, block, send_y.at[d], recv_y.at[d], me, row_peer)

    def copy_c(d):
        block = slots.at[d, own_blk]
        return remote(block, block, send_c.at[d], recv_c.at[d], me, pair_peer)

    def copy_b(d):
        block = slots.at[d, far_blk]
        return remote(block, block, send_b.at[d], recv_b.at[d], me, pair_peer)

    def copy_p(d):
        return remote(
            part.at[d, pl.ds(other_col * 2, 2)],
            pair_in.at[d],
            send_p.at[d],
            recv_p.at[d],
            me,
            pair_peer,
        )

    def copy_q(d):
        return remote(part.at[d, far_blk], col_in.at[d], send_q.at[d], recv_q.at[d], me, row_peer)

    def copy_r(d):
        return remote(
            part.at[d, own_blk], back.at[d], send_r.at[d], recv_r.at[d], partner(d), tp
        )

    @pl.loop(1, n)
    def _(d):
        copy_a(d).start()

        @pl.when(d < near)
        def _():
            copy_n(d).start()

    for fill in fills:
        fill.wait()

    def merge(index, other):
        rows = part.at[index]
        step = min(512, width)

        @pl.loop(0, width // step)
        def _(c):
            cols = pl.ds(pl.multiple_of(c * step, step), step)
            rows[:, cols] = (
                rows[:, cols].astype(jnp.float32) + other[:, cols].astype(jnp.float32)
            ).astype(part.dtype)

    def one_block(rows, put):
        gate = jnp.dot(rows, gate_ref[...], preferred_element_type=jnp.float32)
        up = jnp.dot(rows, up_ref[...], preferred_element_type=jnp.float32)
        hidden_ref[...] = (gate / (1.0 + jnp.exp(-gate)) * up).astype(hidden_ref.dtype)
        step = min(512, width)

        @pl.loop(0, width // step)
        def _(c):
            cols = pl.ds(pl.multiple_of(c * step, step), step)
            put(
                cols,
                jnp.dot(
                    hidden_ref[...], down_ref[:, cols], preferred_element_type=jnp.float32
                ).astype(part.dtype),
            )

    def compute(j):
        if slot_count % 16 == 0:

            def put(cols, val):
                part[j, :, :, cols] = val.reshape(4, slot_count, val.shape[1])

            one_block(slots[j].reshape(4 * slot_count, width), put)
        else:

            @pl.loop(0, 4)
            def _(b):
                def put(cols, val):
                    part[j, b, :, cols] = val

                one_block(slots[j, b], put)

    def inside(j, low):
        return jnp.logical_and(j >= low, j < n)

    @pl.loop(0, n + 5)
    def _(i):
        @pl.when(inside(i, 1))
        def _():
            copy_a(i).wait_recv()
            copy_c(i).start()

        @pl.when(inside(i, near))
        def _():
            copy_y(i).start()

        @pl.when(inside(i - 1, 1))
        def _():
            copy_y(i - 1).wait_recv()
            copy_b(i - 1).start()

        @pl.when(inside(i - 5, 0))
        def _():
            copy_q(i - 5).wait_recv()
            merge((i - 5, own_blk), col_in.at[i - 5])

        @pl.when(inside(i - 3, 0))
        def _():
            copy_p(i - 3).wait_recv()
            for y in range(2):
                merge((i - 3, col * 2 + y), pair_in.at[i - 3, y])

        @pl.when(inside(i - 2, 1))
        def _():
            copy_c(i - 2).wait_recv()
            copy_b(i - 2).wait_recv()

        @pl.when(inside(i - 2, 0))
        def _():
            compute(i - 2)

        @pl.when(inside(i - 5, 1))
        def _():
            copy_r(i - 5).start()

        @pl.when(inside(i - 3, 0))
        def _():
            copy_q(i - 3).start()

        @pl.when(inside(i - 2, 0))
        def _():
            copy_p(i - 2).start()

    def collect(d, rows):
        mix = mix_ref[d]
        high = mix.astype(jnp.bfloat16)
        low = (mix - high.astype(jnp.float32)).astype(jnp.bfloat16)
        both = jnp.dot(high, rows, preferred_element_type=jnp.float32) + jnp.dot(
            low, rows, preferred_element_type=jnp.float32
        )
        return both

    acc[...] = collect(0, part[0, own_blk])

    @pl.loop(1, n)
    def _(d):
        copy_r(d).wait_recv()
        acc[...] += collect(d, back[d])

    res_ref[...] = acc[...].astype(res_ref.dtype)

    @pl.loop(1, n)
    def _(d):
        copy_a(d).wait_send()
        copy_y(d).wait_send()
        copy_c(d).wait_send()
        copy_b(d).wait_send()
        copy_r(d).wait_send()

    @pl.loop(0, n)
    def _(d):
        copy_p(d).wait_send()
        copy_q(d).wait_send()


def run_experts(outgoing, nearby, mine, gate_w, up_w, down_w, mix):
    n, capacity, width = outgoing.shape
    hidden_units = gate_w.shape[1]
    tokens = mix.shape[1]
    rows = 4 * capacity if capacity % 16 == 0 else capacity
    dtype = outgoing.dtype
    vmem = pl.BlockSpec(memory_space=pltpu.VMEM)
    flops = 2 * n * 4 * capacity * width * hidden_units * 3
    return pl.pallas_call(
        functools.partial(expert_kernel, n),
        out_shape=jax.ShapeDtypeStruct((tokens, width), dtype),
        in_specs=[vmem] * 7,
        out_specs=vmem,
        scratch_shapes=[
            pltpu.VMEM((n, 4, capacity, width), dtype),
            pltpu.VMEM((n, 4, capacity, width), dtype),
            pltpu.VMEM((n, 2, capacity, width), dtype),
            pltpu.VMEM((n, capacity, width), dtype),
            pltpu.VMEM((n, capacity, width), dtype),
            pltpu.VMEM((rows, hidden_units), dtype),
            pltpu.VMEM((tokens, width), jnp.float32),
        ]
        + [pltpu.SemaphoreType.DMA((n,))] * 14
        + [pltpu.SemaphoreType.DMA((4,))],
        compiler_params=pltpu.CompilerParams(
            collective_id=0, has_side_effects=True, vmem_limit_bytes=60 * 1024 * 1024
        ),
        cost_estimate=pl.CostEstimate(
            flops=40 * flops, bytes_accessed=16 * 1024 * 1024, transcendentals=0
        ),
    )(outgoing, nearby, mine, gate_w, up_w, down_w, mix)


def expert_part(moe_rows, moe_gain, routes, route_weights, w_gate, w_up, w_down):
    experts = lax.axis_size("ep")
    tp_count = lax.axis_size("tp")
    me = lax.axis_index("ep")
    tp_id = lax.axis_index("tp")
    dev_rows = moe_rows.shape[0] // tp_count
    top_count = routes.shape[1]
    capacity = max(2, 2 * dev_rows * top_count // experts)
    width = moe_rows.shape[1]
    normed = (
        rms_scaled(moe_rows.astype(jnp.float32), moe_gain)
        .astype(jnp.bfloat16)
        .reshape(tp_count, dev_rows, width)
    )
    relative = jnp.bitwise_xor(routes, me).reshape(tp_count, dev_rows, top_count)
    hits = relative[..., None] == lax.iota(jnp.int32, experts)
    named = jnp.any(hits, axis=2)
    before = (
        lax.iota(jnp.int32, dev_rows)[:, None] > lax.iota(jnp.int32, dev_rows)[None, :]
    ).astype(jnp.bfloat16)
    places = jnp.einsum(
        "ij,bjd->bid", before, named.astype(jnp.bfloat16), preferred_element_type=jnp.float32
    ).astype(jnp.int32)
    places = jnp.where(named, places, -1)
    slot_iota = lax.iota(jnp.int32, capacity)
    take_mine = (places[:, None, :, 0] == slot_iota[None, :, None]).astype(jnp.bfloat16)
    mine = jnp.einsum(
        "bst,btm->bsm", take_mine, normed, preferred_element_type=jnp.float32
    ).astype(jnp.bfloat16)
    own = lambda arr: lax.dynamic_index_in_dim(arr, tp_id, 0, keepdims=False)
    other_id = (1 - tp_id // 2) * 2 + tp_id % 2
    own_places = own(places)

    def fill(block, first, last):
        block_places = lax.dynamic_index_in_dim(places, block, 0, keepdims=False)[:, first:last]
        block_rows = lax.dynamic_index_in_dim(normed, block, 0, keepdims=False)
        take = (block_places.T[:, None, :] == slot_iota[None, :, None]).astype(jnp.bfloat16)
        return (
            jnp.dot(
                take.reshape(-1, dev_rows), block_rows, preferred_element_type=jnp.float32
            )
            .astype(jnp.bfloat16)
            .reshape(last - first, capacity, width)
        )

    outgoing = fill(tp_id, 0, experts)
    nearby = fill(other_id, 0, experts // 2)
    own_weights = own(route_weights.reshape(tp_count, dev_rows, top_count))
    weight_of = jnp.sum(jnp.where(own(hits), own_weights[..., None], 0.0), axis=1)
    mix = jnp.where(
        own_places.T[:, :, None] == slot_iota[None, None, :], weight_of.T[:, :, None], 0.0
    )
    return run_experts(outgoing, nearby, mine, w_gate[0], w_up[0], w_down[0], mix)


def local(
    queries,
    keys,
    values,
    attn_lambda,
    head_gain,
    w_out,
    moe_rows,
    moe_gain,
    routes,
    route_weights,
    w_gate,
    w_up,
    w_down,
):
    positions = queries.shape[0]
    q_heads = queries.shape[1]
    kv_heads = keys.shape[1]
    head_dim = queries.shape[2] // 2
    value_dim = values.shape[2]
    per_key = q_heads // kv_heads
    first_pos = lax.axis_index("ep") * positions
    query_pos = first_pos + lax.iota(jnp.int32, positions)
    last_pos = first_pos + positions - 1
    query_view = queries.reshape(positions, kv_heads, per_key, 2, head_dim)
    inv_scale = head_dim ** (-0.5)
    start_max = jnp.full((positions, kv_heads, per_key, 2), MASKED, jnp.float32)
    start_total = jnp.zeros((positions, kv_heads, per_key, 2), jnp.float32)
    start_acc = jnp.zeros((positions, kv_heads, per_key, 2, value_dim), jnp.float32)
    carry = (start_max, start_total, start_acc)
    both = jnp.concatenate([keys, values], axis=2)
    gathered = lax.all_gather(both, "ep", axis=0, tiled=True)
    moe_out = expert_part(moe_rows, moe_gain, routes, route_weights, w_gate, w_up, w_down)
    gathered, moe_out = lax.optimization_barrier((gathered, moe_out))
    key_piece = gathered[:, :, : keys.shape[2]]
    value_piece = gathered[:, :, keys.shape[2] :]
    shard_count = key_piece.shape[0] // positions
    together = 1
    for candidate in (2, 3, 4):
        if shard_count % candidate == 0:
            together = candidate
    block_len = together * positions
    blocks = shard_count // together
    key_blocks = key_piece.reshape(blocks, block_len, kv_heads, 2, head_dim)
    value_blocks = value_piece.reshape(blocks, block_len, kv_heads, value_dim)
    block_starts = block_len * lax.iota(jnp.int32, blocks)

    def visit(running, inputs):
        key_blk, value_blk, block_start = inputs

        def update(current):
            run_max, run_total, run_acc = current
            key_pos = block_start + lax.iota(jnp.int32, block_len)
            scores = (
                jnp.einsum(
                    "qkgmd,pkmd->qkgmp", query_view, key_blk, preferred_element_type=jnp.float32
                )
                * inv_scale
            )
            allowed = key_pos[None, :] <= query_pos[:, None]
            scores = jnp.where(allowed[:, None, None, None, :], scores, MASKED)
            new_max = jnp.maximum(run_max, jnp.max(scores, axis=-1))
            shrink = jnp.exp(run_max - new_max)
            weights = jnp.exp(scores - new_max[..., None])
            run_total = run_total * shrink + jnp.sum(weights, axis=-1)
            run_acc = run_acc * shrink[..., None] + jnp.einsum(
                "qkgmp,pkv->qkgmv",
                weights.astype(jnp.bfloat16),
                value_blk,
                preferred_element_type=jnp.float32,
            )
            return (new_max, run_total, run_acc)

        def keep(current):
            return current

        return (lax.cond(block_start <= last_pos, update, keep, running), None)

    carry, unused = lax.scan(visit, carry, (key_blocks, value_blocks, block_starts))
    run_max, run_total, run_acc = carry
    ratios = run_acc / run_total[..., None]
    lambda_view = attn_lambda.reshape(1, kv_heads, per_key, 1)
    head_out = ratios[:, :, :, 0] - lambda_view * ratios[:, :, :, 1]
    attn_rows = (
        rms_scaled(head_out, head_gain).astype(jnp.bfloat16).reshape(positions, q_heads * value_dim)
    )
    tp_count = lax.axis_size("tp")
    tp_id = lax.axis_index("tp")
    exchanged = lax.all_to_all(
        attn_rows.reshape(positions, q_heads, value_dim),
        "tp",
        split_axis=0,
        concat_axis=1,
        tiled=True,
    )
    mixer_out = jnp.dot(
        exchanged.reshape(positions // tp_count, tp_count * q_heads * value_dim),
        w_out,
        preferred_element_type=jnp.float32,
    ).astype(jnp.bfloat16)
    return (mixer_out, moe_out)


def solution(mesh):
    return jax.shard_map(
        local,
        mesh=mesh,
        in_specs=(
            P("ep", "tp", None),
            P("ep", "tp", None),
            P("ep", "tp", None),
            P("tp"),
            P(),
            P(),
            P("ep", None),
            P(),
            P("ep", None),
            P("ep", None),
            P("ep", None, "tp"),
            P("ep", None, "tp"),
            P("ep", "tp", None),
        ),
        out_specs=(P(("ep", "tp"), None), P(("ep", "tp"), None)),
        check_vma=False,
    )
```

```python
import functools

import jax
import jax.numpy as jnp
from jax import lax
from jax.experimental import pallas as pl
from jax.experimental.pallas import tpu as pltpu
from jax.sharding import PartitionSpec as P

EPSILON = 1e-06
MASKED = -1e30


def rms_scaled(values_f, gain):
    mean_sq = jnp.mean(values_f * values_f, axis=-1, keepdims=True)
    return values_f * lax.rsqrt(mean_sq + EPSILON) * gain


def expert_kernel(
    n,
    out_ref,
    near_ref,
    rows_ref,
    take_ref,
    mine_ref,
    gate_ref,
    up_ref,
    down_ref,
    mix_ref,
    res_ref,
    slots,
    part,
    pair_in,
    col_in,
    back,
    far_rows,
    far_take,
    picked,
    hidden_ref,
    acc,
    send_s,
    recv_s,
    send_a,
    recv_a,
    send_y,
    recv_y,
    send_c,
    recv_c,
    send_b,
    recv_b,
    send_p,
    recv_p,
    send_q,
    recv_q,
    send_r,
    recv_r,
    local_sem,
):
    me = lax.axis_index("ep")
    tp = lax.axis_index("tp")
    row = tp // 2
    col = tp % 2
    other_row = 1 - row
    other_col = 1 - col
    pair_peer = row * 2 + other_col
    row_peer = other_row * 2 + col
    own_blk = col * 2 + row
    far_blk = col * 2 + other_row
    slot_count = slots.shape[2]
    width = slots.shape[3]

    near = near_ref.shape[0]
    half = out_ref.shape[0]
    bubble = 3
    bits = [1 << b for b in range(n.bit_length() - 1)]

    def partner(d):
        total = 0
        for bit in bits:
            total = total + (me // bit + d // bit) % 2 * bit
        return total

    def remote(src, dst, ssem, rsem, ep_id, tp_id):
        return pltpu.make_async_remote_copy(
            src_ref=src,
            dst_ref=dst,
            send_sem=ssem,
            recv_sem=rsem,
            device_id=(ep_id, tp_id),
            device_id_type=pl.DeviceIdType.MESH,
        )

    barrier = pltpu.get_barrier_semaphore()

    @pl.loop(1, n)
    def _(d):
        pl.semaphore_signal(
            barrier, inc=1, device_id=(partner(d), tp), device_id_type=pl.DeviceIdType.MESH
        )

    for peer in (pair_peer, row_peer):
        pl.semaphore_signal(
            barrier, inc=1, device_id=(me, peer), device_id_type=pl.DeviceIdType.MESH
        )
    fills = [
        pltpu.make_async_copy(
            mine_ref.at[b], slots.at[0, (b % 2) * 2 + b // 2], local_sem.at[b]
        )
        for b in range(4)
    ]
    for fill in fills:
        fill.start()
    pl.semaphore_wait(barrier, n + 1)

    def copy_a(d):
        return remote(
            out_ref.at[d], slots.at[d, own_blk], send_a.at[d], recv_a.at[d], partner(d), tp
        )

    def copy_s():
        return [
            remote(src, dst, send_s.at[k], recv_s.at[k], partner(half), tp)
            for k, (src, dst) in enumerate(((take_ref, far_take), (rows_ref, far_rows)))
        ]

    def copy_g(d):
        return remote(
            picked.at[d - half],
            slots.at[d, own_blk],
            send_a.at[d],
            recv_a.at[d],
            partner(d - half),
            tp,
        )

    def copy_n(d):
        return remote(
            near_ref.at[d], slots.at[d, far_blk], send_y.at[d], recv_y.at[d], partner(d), tp
        )

    def copy_y(d):
        block = slots.at[d, own_blk]
        return remote(block, block, send_y.at[d], recv_y.at[d], me, row_peer)

    def copy_c(d):
        block = slots.at[d, own_blk]
        return remote(block, block, send_c.at[d], recv_c.at[d], me, pair_peer)

    def copy_b(d):
        block = slots.at[d, far_blk]
        return remote(block, block, send_b.at[d], recv_b.at[d], me, pair_peer)

    def copy_p(d):
        return remote(
            part.at[d, pl.ds(other_col * 2, 2)],
            pair_in.at[d],
            send_p.at[d],
            recv_p.at[d],
            me,
            pair_peer,
        )

    def copy_q(d):
        return remote(part.at[d, far_blk], col_in.at[d], send_q.at[d], recv_q.at[d], me, row_peer)

    def copy_r(d):
        return remote(
            part.at[d, own_blk], back.at[d], send_r.at[d], recv_r.at[d], partner(d), tp
        )

    for swap in copy_s():
        swap.start()

    @pl.loop(1, half)
    def _(d):
        copy_a(d).start()

        @pl.when(d < near)
        def _():
            copy_n(d).start()

    for fill in fills:
        fill.wait()

    def merge(index, other):
        rows = part.at[index]
        step = min(512, width)

        @pl.loop(0, width // step)
        def _(c):
            cols = pl.ds(pl.multiple_of(c * step, step), step)
            rows[:, cols] = (
                rows[:, cols].astype(jnp.float32) + other[:, cols].astype(jnp.float32)
            ).astype(part.dtype)

    def one_block(rows, put):
        gate = jnp.dot(rows, gate_ref[...], preferred_element_type=jnp.float32)
        up = jnp.dot(rows, up_ref[...], preferred_element_type=jnp.float32)
        hidden_ref[...] = (gate / (1.0 + jnp.exp(-gate)) * up).astype(hidden_ref.dtype)
        step = min(512, width)

        @pl.loop(0, width // step)
        def _(c):
            cols = pl.ds(pl.multiple_of(c * step, step), step)
            put(
                cols,
                jnp.dot(
                    hidden_ref[...], down_ref[:, cols], preferred_element_type=jnp.float32
                ).astype(part.dtype),
            )

    def compute(j):
        if slot_count % 16 == 0:

            def put(cols, val):
                part[j, :, :, cols] = val.reshape(4, slot_count, val.shape[1])

            one_block(slots[j].reshape(4 * slot_count, width), put)
        else:

            @pl.loop(0, 4)
            def _(b):
                def put(cols, val):
                    part[j, b, :, cols] = val

                one_block(slots[j, b], put)

    def pick():
        for swap in copy_s():
            swap.wait_recv()
        step = min(512, width)

        @pl.loop(0, width // step)
        def _(c):
            cols = pl.ds(pl.multiple_of(c * step, step), step)
            rows = jnp.dot(
                far_take[...], far_rows[:, cols], preferred_element_type=jnp.float32
            )
            rows = rows.reshape(half, slot_count, step).astype(picked.dtype)
            picked[:, :, cols] = rows
            slots[half, own_blk, :, cols] = rows[0]

        @pl.loop(half + 1, n)
        def _(d):
            copy_g(d).start()

    def at_stage(k, low, action):
        j = k - bubble * (k // (half + bubble))

        @pl.when(
            jnp.logical_or(
                jnp.logical_and(k >= low, k < half),
                jnp.logical_and(k >= max(low, half) + bubble, k < n + bubble),
            )
        )
        def _():
            action(j)

    def arrive(j):
        @pl.when(j < half)
        def _():
            copy_a(j).wait_recv()

        @pl.when(j == half)
        def _():
            pick()

        @pl.when(j > half)
        def _():
            copy_g(j).wait_recv()

        copy_c(j).start()

        @pl.when(j >= near)
        def _():
            copy_y(j).start()

    def cross(j):
        copy_y(j).wait_recv()
        copy_b(j).start()

    def finish(j):
        copy_q(j).wait_recv()
        merge((j, own_blk), col_in.at[j])

    def join(j):
        copy_p(j).wait_recv()
        for y in range(2):
            merge((j, col * 2 + y), pair_in.at[j, y])

    def ready(j):
        copy_c(j).wait_recv()
        copy_b(j).wait_recv()

    @pl.loop(0, n + 5 + bubble)
    def _(i):
        at_stage(i, 1, arrive)
        at_stage(i - 1, 1, cross)
        at_stage(i - 5, 0, finish)
        at_stage(i - 3, 0, join)
        at_stage(i - 2, 1, ready)
        at_stage(i - 2, 0, compute)
        at_stage(i - 5, 1, lambda j: copy_r(j).start())
        at_stage(i - 3, 0, lambda j: copy_q(j).start())
        at_stage(i - 2, 0, lambda j: copy_p(j).start())

    def collect(d, rows):
        mix = mix_ref[d]
        high = mix.astype(jnp.bfloat16)
        low = (mix - high.astype(jnp.float32)).astype(jnp.bfloat16)
        both = jnp.dot(high, rows, preferred_element_type=jnp.float32) + jnp.dot(
            low, rows, preferred_element_type=jnp.float32
        )
        return both

    acc[...] = collect(0, part[0, own_blk])

    @pl.loop(1, n)
    def _(d):
        copy_r(d).wait_recv()
        acc[...] += collect(d, back[d])

    res_ref[...] = acc[...].astype(res_ref.dtype)

    for swap in copy_s():
        swap.wait_send()

    @pl.loop(1, half)
    def _(d):
        copy_a(d).wait_send()

    @pl.loop(half + 1, n)
    def _(d):
        copy_g(d).wait_send()

    @pl.loop(1, n)
    def _(d):
        copy_y(d).wait_send()
        copy_c(d).wait_send()
        copy_b(d).wait_send()
        copy_r(d).wait_send()

    @pl.loop(0, n)
    def _(d):
        copy_p(d).wait_send()
        copy_q(d).wait_send()


def run_experts(n, outgoing, nearby, own_rows, far_take, mine, gate_w, up_w, down_w, mix):
    half, capacity, width = outgoing.shape
    hidden_units = gate_w.shape[1]
    tokens = mix.shape[1]
    rows = 4 * capacity if capacity % 16 == 0 else capacity
    dtype = outgoing.dtype
    vmem = pl.BlockSpec(memory_space=pltpu.VMEM)
    flops = 2 * n * 4 * capacity * width * hidden_units * 3
    return pl.pallas_call(
        functools.partial(expert_kernel, n),
        out_shape=jax.ShapeDtypeStruct((tokens, width), dtype),
        in_specs=[vmem] * 9,
        out_specs=vmem,
        scratch_shapes=[
            pltpu.VMEM((n, 4, capacity, width), dtype),
            pltpu.VMEM((n, 4, capacity, width), dtype),
            pltpu.VMEM((n, 2, capacity, width), dtype),
            pltpu.VMEM((n, capacity, width), dtype),
            pltpu.VMEM((n, capacity, width), dtype),
            pltpu.VMEM(own_rows.shape, dtype),
            pltpu.VMEM(far_take.shape, dtype),
            pltpu.VMEM((half, capacity, width), dtype),
            pltpu.VMEM((rows, hidden_units), dtype),
            pltpu.VMEM((tokens, width), jnp.float32),
        ]
        + [pltpu.SemaphoreType.DMA((2,))] * 2
        + [pltpu.SemaphoreType.DMA((n,))] * 14
        + [pltpu.SemaphoreType.DMA((4,))],
        compiler_params=pltpu.CompilerParams(
            collective_id=0, has_side_effects=True, vmem_limit_bytes=60 * 1024 * 1024
        ),
        cost_estimate=pl.CostEstimate(
            flops=40 * flops, bytes_accessed=16 * 1024 * 1024, transcendentals=0
        ),
    )(outgoing, nearby, own_rows, far_take, mine, gate_w, up_w, down_w, mix)


def expert_part(moe_rows, moe_gain, routes, route_weights, w_gate, w_up, w_down):
    experts = lax.axis_size("ep")
    tp_count = lax.axis_size("tp")
    me = lax.axis_index("ep")
    tp_id = lax.axis_index("tp")
    dev_rows = moe_rows.shape[0] // tp_count
    top_count = routes.shape[1]
    capacity = max(2, 2 * dev_rows * top_count // experts)
    width = moe_rows.shape[1]
    normed = (
        rms_scaled(moe_rows.astype(jnp.float32), moe_gain)
        .astype(jnp.bfloat16)
        .reshape(tp_count, dev_rows, width)
    )
    relative = jnp.bitwise_xor(routes, me).reshape(tp_count, dev_rows, top_count)
    hits = relative[..., None] == lax.iota(jnp.int32, experts)
    named = jnp.any(hits, axis=2)
    before = (
        lax.iota(jnp.int32, dev_rows)[:, None] > lax.iota(jnp.int32, dev_rows)[None, :]
    ).astype(jnp.bfloat16)
    places = jnp.einsum(
        "ij,bjd->bid", before, named.astype(jnp.bfloat16), preferred_element_type=jnp.float32
    ).astype(jnp.int32)
    places = jnp.where(named, places, -1)
    slot_iota = lax.iota(jnp.int32, capacity)
    take_mine = (places[:, None, :, 0] == slot_iota[None, :, None]).astype(jnp.bfloat16)
    mine = jnp.einsum(
        "bst,btm->bsm", take_mine, normed, preferred_element_type=jnp.float32
    ).astype(jnp.bfloat16)
    own = lambda arr: lax.dynamic_index_in_dim(arr, tp_id, 0, keepdims=False)
    other_id = (1 - tp_id // 2) * 2 + tp_id % 2
    own_places = own(places)

    half = experts // 2

    def takes(block_places):
        hits = block_places.T[:, None, :] == slot_iota[None, :, None]
        return hits.astype(jnp.bfloat16).reshape(-1, dev_rows)

    def fill(take, block_rows):
        filled = jnp.dot(take, block_rows, preferred_element_type=jnp.float32)
        return filled.astype(jnp.bfloat16).reshape(-1, capacity, width)

    own_rows = own(normed)
    own_take = takes(own_places)
    outgoing = fill(own_take[: half * capacity], own_rows)
    far_take = own_take[half * capacity :]
    near = max(2, half - 1)
    nearby = fill(
        takes(lax.dynamic_index_in_dim(places, other_id, 0, keepdims=False)[:, :near]),
        lax.dynamic_index_in_dim(normed, other_id, 0, keepdims=False),
    )
    own_weights = own(route_weights.reshape(tp_count, dev_rows, top_count))
    weight_of = jnp.sum(jnp.where(own(hits), own_weights[..., None], 0.0), axis=1)
    mix = jnp.where(
        own_places.T[:, :, None] == slot_iota[None, None, :], weight_of.T[:, :, None], 0.0
    )
    return run_experts(
        experts, outgoing, nearby, own_rows, far_take, mine, w_gate[0], w_up[0], w_down[0], mix
    )


def local(
    queries,
    keys,
    values,
    attn_lambda,
    head_gain,
    w_out,
    moe_rows,
    moe_gain,
    routes,
    route_weights,
    w_gate,
    w_up,
    w_down,
):
    positions = queries.shape[0]
    q_heads = queries.shape[1]
    kv_heads = keys.shape[1]
    head_dim = queries.shape[2] // 2
    value_dim = values.shape[2]
    per_key = q_heads // kv_heads
    first_pos = lax.axis_index("ep") * positions
    query_pos = first_pos + lax.iota(jnp.int32, positions)
    last_pos = first_pos + positions - 1
    query_view = queries.reshape(positions, kv_heads, per_key, 2, head_dim)
    inv_scale = head_dim ** (-0.5)
    start_max = jnp.full((positions, kv_heads, per_key, 2), MASKED, jnp.float32)
    start_total = jnp.zeros((positions, kv_heads, per_key, 2), jnp.float32)
    start_acc = jnp.zeros((positions, kv_heads, per_key, 2, value_dim), jnp.float32)
    carry = (start_max, start_total, start_acc)
    both = jnp.concatenate([keys, values], axis=2)
    gathered = lax.all_gather(both, "ep", axis=0, tiled=True)
    moe_out = expert_part(moe_rows, moe_gain, routes, route_weights, w_gate, w_up, w_down)
    gathered, moe_out = lax.optimization_barrier((gathered, moe_out))
    key_piece = gathered[:, :, : keys.shape[2]]
    value_piece = gathered[:, :, keys.shape[2] :]
    shard_count = key_piece.shape[0] // positions
    together = 1
    for candidate in (2, 3, 4):
        if shard_count % candidate == 0:
            together = candidate
    block_len = together * positions
    blocks = shard_count // together
    key_blocks = key_piece.reshape(blocks, block_len, kv_heads, 2, head_dim)
    value_blocks = value_piece.reshape(blocks, block_len, kv_heads, value_dim)
    block_starts = block_len * lax.iota(jnp.int32, blocks)

    def visit(running, inputs):
        key_blk, value_blk, block_start = inputs

        def update(current):
            run_max, run_total, run_acc = current
            key_pos = block_start + lax.iota(jnp.int32, block_len)
            scores = (
                jnp.einsum(
                    "qkgmd,pkmd->qkgmp", query_view, key_blk, preferred_element_type=jnp.float32
                )
                * inv_scale
            )
            allowed = key_pos[None, :] <= query_pos[:, None]
            scores = jnp.where(allowed[:, None, None, None, :], scores, MASKED)
            new_max = jnp.maximum(run_max, jnp.max(scores, axis=-1))
            shrink = jnp.exp(run_max - new_max)
            weights = jnp.exp(scores - new_max[..., None])
            run_total = run_total * shrink + jnp.sum(weights, axis=-1)
            run_acc = run_acc * shrink[..., None] + jnp.einsum(
                "qkgmp,pkv->qkgmv",
                weights.astype(jnp.bfloat16),
                value_blk,
                preferred_element_type=jnp.float32,
            )
            return (new_max, run_total, run_acc)

        def keep(current):
            return current

        return (lax.cond(block_start <= last_pos, update, keep, running), None)

    carry, unused = lax.scan(visit, carry, (key_blocks, value_blocks, block_starts))
    run_max, run_total, run_acc = carry
    ratios = run_acc / run_total[..., None]
    lambda_view = attn_lambda.reshape(1, kv_heads, per_key, 1)
    head_out = ratios[:, :, :, 0] - lambda_view * ratios[:, :, :, 1]
    attn_rows = (
        rms_scaled(head_out, head_gain).astype(jnp.bfloat16).reshape(positions, q_heads * value_dim)
    )
    tp_count = lax.axis_size("tp")
    tp_id = lax.axis_index("tp")
    exchanged = lax.all_to_all(
        attn_rows.reshape(positions, q_heads, value_dim),
        "tp",
        split_axis=0,
        concat_axis=1,
        tiled=True,
    )
    mixer_out = jnp.dot(
        exchanged.reshape(positions // tp_count, tp_count * q_heads * value_dim),
        w_out,
        preferred_element_type=jnp.float32,
    ).astype(jnp.bfloat16)
    return (mixer_out, moe_out)


def solution(mesh):
    return jax.shard_map(
        local,
        mesh=mesh,
        in_specs=(
            P("ep", "tp", None),
            P("ep", "tp", None),
            P("ep", "tp", None),
            P("tp"),
            P(),
            P(),
            P("ep", None),
            P(),
            P("ep", None),
            P("ep", None),
            P("ep", None, "tp"),
            P("ep", None, "tp"),
            P("ep", "tp", None),
        ),
        out_specs=(P(("ep", "tp"), None), P(("ep", "tp"), None)),
        check_vma=False,
    )
```

```python
import functools

import jax
import jax.numpy as jnp
from jax import lax
from jax.experimental import pallas as pl
from jax.experimental.pallas import tpu as pltpu
from jax.sharding import PartitionSpec as P

EPSILON = 1e-06
MASKED = -1e30


def rms_scaled(values_f, gain):
    mean_sq = jnp.mean(values_f * values_f, axis=-1, keepdims=True)
    return values_f * lax.rsqrt(mean_sq + EPSILON) * gain


def expert_kernel(
    n,
    out_ref,
    near_ref,
    mine_ref,
    kv_ref,
    gate_ref,
    up_ref,
    down_ref,
    mix_ref,
    res_ref,
    kv_out,
    slots,
    part,
    pair_in,
    col_in,
    back,
    hidden_ref,
    acc,
    send_k,
    recv_k,
    send_a,
    recv_a,
    send_y,
    recv_y,
    send_c,
    recv_c,
    send_b,
    recv_b,
    send_p,
    recv_p,
    send_q,
    recv_q,
    send_r,
    recv_r,
    local_sem,
):
    me = lax.axis_index("ep")
    tp = lax.axis_index("tp")
    row = tp // 2
    col = tp % 2
    other_row = 1 - row
    other_col = 1 - col
    pair_peer = row * 2 + other_col
    row_peer = other_row * 2 + col
    own_blk = col * 2 + row
    far_blk = col * 2 + other_row
    slot_count = slots.shape[2]
    width = slots.shape[3]

    near = near_ref.shape[0]
    bits = [1 << b for b in range(n.bit_length() - 1)]

    def partner(d):
        total = 0
        for bit in bits:
            total = total + (me // bit + d // bit) % 2 * bit
        return total

    def remote(src, dst, ssem, rsem, ep_id, tp_id):
        return pltpu.make_async_remote_copy(
            src_ref=src,
            dst_ref=dst,
            send_sem=ssem,
            recv_sem=rsem,
            device_id=(ep_id, tp_id),
            device_id_type=pl.DeviceIdType.MESH,
        )

    barrier = pltpu.get_barrier_semaphore()

    @pl.loop(1, n)
    def _(d):
        pl.semaphore_signal(
            barrier, inc=1, device_id=(partner(d), tp), device_id_type=pl.DeviceIdType.MESH
        )

    for peer in (pair_peer, row_peer):
        pl.semaphore_signal(
            barrier, inc=1, device_id=(me, peer), device_id_type=pl.DeviceIdType.MESH
        )
    keep = pltpu.make_async_copy(kv_ref, kv_out.at[me], local_sem.at[4])
    keep.start()
    fills = [
        pltpu.make_async_copy(
            mine_ref.at[b], slots.at[0, (b % 2) * 2 + b // 2], local_sem.at[b]
        )
        for b in range(4)
    ]
    for fill in fills:
        fill.start()
    pl.semaphore_wait(barrier, n + 1)

    def copy_a(d):
        return remote(
            out_ref.at[d], slots.at[d, own_blk], send_a.at[d], recv_a.at[d], partner(d), tp
        )

    def copy_k(d):
        return remote(kv_ref, kv_out.at[me], send_k.at[d], recv_k.at[d], partner(d), tp)

    def copy_f(d):
        block = kv_out.at[partner(near)]
        return remote(block, block, send_k.at[d], recv_k.at[d], partner(d - near), tp)

    def copy_n(d):
        return remote(
            near_ref.at[d], slots.at[d, far_blk], send_y.at[d], recv_y.at[d], partner(d), tp
        )

    def copy_y(d):
        block = slots.at[d, own_blk]
        return remote(block, block, send_y.at[d], recv_y.at[d], me, row_peer)

    def copy_c(d):
        block = slots.at[d, own_blk]
        return remote(block, block, send_c.at[d], recv_c.at[d], me, pair_peer)

    def copy_b(d):
        block = slots.at[d, far_blk]
        return remote(block, block, send_b.at[d], recv_b.at[d], me, pair_peer)

    def copy_p(d):
        return remote(
            part.at[d, pl.ds(other_col * 2, 2)],
            pair_in.at[d],
            send_p.at[d],
            recv_p.at[d],
            me,
            pair_peer,
        )

    def copy_q(d):
        return remote(part.at[d, far_blk], col_in.at[d], send_q.at[d], recv_q.at[d], me, row_peer)

    def copy_r(d):
        return remote(
            part.at[d, own_blk], back.at[d], send_r.at[d], recv_r.at[d], partner(d), tp
        )

    @pl.loop(1, n)
    def _(d):
        copy_a(d).start()

        @pl.when(d < near)
        def _():
            copy_n(d).start()

    copy_k(near).start()

    @pl.loop(1, near)
    def _(d):
        copy_k(d).start()

    for fill in fills:
        fill.wait()

    def merge(index, other):
        rows = part.at[index]
        step = min(512, width)

        @pl.loop(0, width // step)
        def _(c):
            cols = pl.ds(pl.multiple_of(c * step, step), step)
            rows[:, cols] = (
                rows[:, cols].astype(jnp.float32) + other[:, cols].astype(jnp.float32)
            ).astype(part.dtype)

    def one_block(rows, put):
        gate = jnp.dot(rows, gate_ref[...], preferred_element_type=jnp.float32)
        up = jnp.dot(rows, up_ref[...], preferred_element_type=jnp.float32)
        hidden_ref[...] = (gate / (1.0 + jnp.exp(-gate)) * up).astype(hidden_ref.dtype)
        step = min(512, width)

        @pl.loop(0, width // step)
        def _(c):
            cols = pl.ds(pl.multiple_of(c * step, step), step)
            put(
                cols,
                jnp.dot(
                    hidden_ref[...], down_ref[:, cols], preferred_element_type=jnp.float32
                ).astype(part.dtype),
            )

    def compute(j):
        if slot_count % 16 == 0:

            def put(cols, val):
                part[j, :, :, cols] = val.reshape(4, slot_count, val.shape[1])

            one_block(slots[j].reshape(4 * slot_count, width), put)
        else:

            @pl.loop(0, 4)
            def _(b):
                def put(cols, val):
                    part[j, b, :, cols] = val

                one_block(slots[j, b], put)

    def inside(j, low):
        return jnp.logical_and(j >= low, j < n)

    @pl.loop(0, n + 5)
    def _(i):
        @pl.when(inside(i, 1))
        def _():
            copy_a(i).wait_recv()
            copy_c(i).start()

        @pl.when(inside(i, near))
        def _():
            copy_y(i).start()

        @pl.when(i == near)
        def _():
            copy_k(near).wait_recv()

            @pl.loop(near + 1, n)
            def _(d):
                copy_f(d).start()

        @pl.when(inside(i - 1, 1))
        def _():
            copy_y(i - 1).wait_recv()
            copy_b(i - 1).start()

        @pl.when(inside(i - 5, 0))
        def _():
            copy_q(i - 5).wait_recv()
            merge((i - 5, own_blk), col_in.at[i - 5])

        @pl.when(inside(i - 3, 0))
        def _():
            copy_p(i - 3).wait_recv()
            for y in range(2):
                merge((i - 3, col * 2 + y), pair_in.at[i - 3, y])

        @pl.when(inside(i - 2, 1))
        def _():
            copy_c(i - 2).wait_recv()
            copy_b(i - 2).wait_recv()

        @pl.when(inside(i - 2, 0))
        def _():
            compute(i - 2)

        @pl.when(inside(i - 5, 1))
        def _():
            copy_r(i - 5).start()

        @pl.when(inside(i - 3, 0))
        def _():
            copy_q(i - 3).start()

        @pl.when(inside(i - 2, 0))
        def _():
            copy_p(i - 2).start()

    def collect(d, rows):
        mix = mix_ref[d]
        high = mix.astype(jnp.bfloat16)
        low = (mix - high.astype(jnp.float32)).astype(jnp.bfloat16)
        both = jnp.dot(high, rows, preferred_element_type=jnp.float32) + jnp.dot(
            low, rows, preferred_element_type=jnp.float32
        )
        return both

    acc[...] = collect(0, part[0, own_blk])

    @pl.loop(1, n)
    def _(d):
        copy_r(d).wait_recv()
        acc[...] += collect(d, back[d])

    @pl.loop(1, near)
    def _(d):
        copy_k(d).wait()

    copy_k(near).wait_send()

    @pl.loop(near + 1, n)
    def _(d):
        copy_f(d).wait()

    keep.wait()
    res_ref[...] = acc[...].astype(res_ref.dtype)

    @pl.loop(1, n)
    def _(d):
        copy_a(d).wait_send()
        copy_y(d).wait_send()
        copy_c(d).wait_send()
        copy_b(d).wait_send()
        copy_r(d).wait_send()

    @pl.loop(0, n)
    def _(d):
        copy_p(d).wait_send()
        copy_q(d).wait_send()


def run_experts(outgoing, nearby, mine, kv, gate_w, up_w, down_w, mix):
    n, capacity, width = outgoing.shape
    hidden_units = gate_w.shape[1]
    tokens = mix.shape[1]
    rows = 4 * capacity if capacity % 16 == 0 else capacity
    dtype = outgoing.dtype
    vmem = pl.BlockSpec(memory_space=pltpu.VMEM)
    flops = 2 * n * 4 * capacity * width * hidden_units * 3
    return pl.pallas_call(
        functools.partial(expert_kernel, n),
        out_shape=(
            jax.ShapeDtypeStruct((tokens, width), dtype),
            jax.ShapeDtypeStruct((n,) + kv.shape, kv.dtype),
        ),
        in_specs=[vmem] * 8,
        out_specs=(vmem, pl.BlockSpec(memory_space=pl.ANY)),
        scratch_shapes=[
            pltpu.VMEM((n, 4, capacity, width), dtype),
            pltpu.VMEM((n, 4, capacity, width), dtype),
            pltpu.VMEM((n, 2, capacity, width), dtype),
            pltpu.VMEM((n, capacity, width), dtype),
            pltpu.VMEM((n, capacity, width), dtype),
            pltpu.VMEM((rows, hidden_units), dtype),
            pltpu.VMEM((tokens, width), jnp.float32),
        ]
        + [pltpu.SemaphoreType.DMA((n,))] * 16
        + [pltpu.SemaphoreType.DMA((5,))],
        compiler_params=pltpu.CompilerParams(
            collective_id=0, has_side_effects=True, vmem_limit_bytes=60 * 1024 * 1024
        ),
        cost_estimate=pl.CostEstimate(
            flops=40 * flops, bytes_accessed=16 * 1024 * 1024, transcendentals=0
        ),
    )(outgoing, nearby, mine, kv, gate_w, up_w, down_w, mix)


def expert_part(kv, moe_rows, moe_gain, routes, route_weights, w_gate, w_up, w_down):
    experts = lax.axis_size("ep")
    tp_count = lax.axis_size("tp")
    me = lax.axis_index("ep")
    tp_id = lax.axis_index("tp")
    dev_rows = moe_rows.shape[0] // tp_count
    top_count = routes.shape[1]
    capacity = max(2, 2 * dev_rows * top_count // experts)
    width = moe_rows.shape[1]
    normed = (
        rms_scaled(moe_rows.astype(jnp.float32), moe_gain)
        .astype(jnp.bfloat16)
        .reshape(tp_count, dev_rows, width)
    )
    relative = jnp.bitwise_xor(routes, me).reshape(tp_count, dev_rows, top_count)
    hits = relative[..., None] == lax.iota(jnp.int32, experts)
    named = jnp.any(hits, axis=2)
    before = (
        lax.iota(jnp.int32, dev_rows)[:, None] > lax.iota(jnp.int32, dev_rows)[None, :]
    ).astype(jnp.bfloat16)
    places = jnp.einsum(
        "ij,bjd->bid", before, named.astype(jnp.bfloat16), preferred_element_type=jnp.float32
    ).astype(jnp.int32)
    places = jnp.where(named, places, -1)
    slot_iota = lax.iota(jnp.int32, capacity)
    take_mine = (places[:, None, :, 0] == slot_iota[None, :, None]).astype(jnp.bfloat16)
    mine = jnp.einsum(
        "bst,btm->bsm", take_mine, normed, preferred_element_type=jnp.float32
    ).astype(jnp.bfloat16)
    own = lambda arr: lax.dynamic_index_in_dim(arr, tp_id, 0, keepdims=False)
    other_id = (1 - tp_id // 2) * 2 + tp_id % 2
    own_places = own(places)

    def fill(block, first, last):
        block_places = lax.dynamic_index_in_dim(places, block, 0, keepdims=False)[:, first:last]
        block_rows = lax.dynamic_index_in_dim(normed, block, 0, keepdims=False)
        take = (block_places.T[:, None, :] == slot_iota[None, :, None]).astype(jnp.bfloat16)
        return (
            jnp.dot(
                take.reshape(-1, dev_rows), block_rows, preferred_element_type=jnp.float32
            )
            .astype(jnp.bfloat16)
            .reshape(last - first, capacity, width)
        )

    outgoing = fill(tp_id, 0, experts)
    nearby = fill(other_id, 0, experts // 2)
    own_weights = own(route_weights.reshape(tp_count, dev_rows, top_count))
    weight_of = jnp.sum(jnp.where(own(hits), own_weights[..., None], 0.0), axis=1)
    mix = jnp.where(
        own_places.T[:, :, None] == slot_iota[None, None, :], weight_of.T[:, :, None], 0.0
    )
    return run_experts(outgoing, nearby, mine, kv, w_gate[0], w_up[0], w_down[0], mix)


def local(
    queries,
    keys,
    values,
    attn_lambda,
    head_gain,
    w_out,
    moe_rows,
    moe_gain,
    routes,
    route_weights,
    w_gate,
    w_up,
    w_down,
):
    positions = queries.shape[0]
    q_heads = queries.shape[1]
    kv_heads = keys.shape[1]
    head_dim = queries.shape[2] // 2
    value_dim = values.shape[2]
    per_key = q_heads // kv_heads
    first_pos = lax.axis_index("ep") * positions
    query_pos = first_pos + lax.iota(jnp.int32, positions)
    last_pos = first_pos + positions - 1
    query_view = queries.reshape(positions, kv_heads, per_key, 2, head_dim)
    inv_scale = head_dim ** (-0.5)
    start_max = jnp.full((positions, kv_heads, per_key, 2), MASKED, jnp.float32)
    start_total = jnp.zeros((positions, kv_heads, per_key, 2), jnp.float32)
    start_acc = jnp.zeros((positions, kv_heads, per_key, 2, value_dim), jnp.float32)
    carry = (start_max, start_total, start_acc)
    both = jnp.concatenate([keys, values], axis=2)
    moe_out, gathered = expert_part(
        both.reshape(positions, -1),
        moe_rows,
        moe_gain,
        routes,
        route_weights,
        w_gate,
        w_up,
        w_down,
    )
    gathered = gathered.reshape(-1, kv_heads, both.shape[2])
    key_piece = gathered[:, :, : keys.shape[2]]
    value_piece = gathered[:, :, keys.shape[2] :]
    shard_count = key_piece.shape[0] // positions
    together = 1
    for candidate in (2, 3, 4):
        if shard_count % candidate == 0:
            together = candidate
    block_len = together * positions
    blocks = shard_count // together
    key_blocks = key_piece.reshape(blocks, block_len, kv_heads, 2, head_dim)
    value_blocks = value_piece.reshape(blocks, block_len, kv_heads, value_dim)
    block_starts = block_len * lax.iota(jnp.int32, blocks)

    def visit(running, inputs):
        key_blk, value_blk, block_start = inputs

        def update(current):
            run_max, run_total, run_acc = current
            key_pos = block_start + lax.iota(jnp.int32, block_len)
            scores = (
                jnp.einsum(
                    "qkgmd,pkmd->qkgmp", query_view, key_blk, preferred_element_type=jnp.float32
                )
                * inv_scale
            )
            allowed = key_pos[None, :] <= query_pos[:, None]
            scores = jnp.where(allowed[:, None, None, None, :], scores, MASKED)
            new_max = jnp.maximum(run_max, jnp.max(scores, axis=-1))
            shrink = jnp.exp(run_max - new_max)
            weights = jnp.exp(scores - new_max[..., None])
            run_total = run_total * shrink + jnp.sum(weights, axis=-1)
            run_acc = run_acc * shrink[..., None] + jnp.einsum(
                "qkgmp,pkv->qkgmv",
                weights.astype(jnp.bfloat16),
                value_blk,
                preferred_element_type=jnp.float32,
            )
            return (new_max, run_total, run_acc)

        def keep(current):
            return current

        return (lax.cond(block_start <= last_pos, update, keep, running), None)

    carry, unused = lax.scan(visit, carry, (key_blocks, value_blocks, block_starts))
    run_max, run_total, run_acc = carry
    ratios = run_acc / run_total[..., None]
    lambda_view = attn_lambda.reshape(1, kv_heads, per_key, 1)
    head_out = ratios[:, :, :, 0] - lambda_view * ratios[:, :, :, 1]
    attn_rows = (
        rms_scaled(head_out, head_gain).astype(jnp.bfloat16).reshape(positions, q_heads * value_dim)
    )
    tp_count = lax.axis_size("tp")
    tp_id = lax.axis_index("tp")
    exchanged = lax.all_to_all(
        attn_rows.reshape(positions, q_heads, value_dim),
        "tp",
        split_axis=0,
        concat_axis=1,
        tiled=True,
    )
    mixer_out = jnp.dot(
        exchanged.reshape(positions // tp_count, tp_count * q_heads * value_dim),
        w_out,
        preferred_element_type=jnp.float32,
    ).astype(jnp.bfloat16)
    return (mixer_out, moe_out)


def solution(mesh):
    return jax.shard_map(
        local,
        mesh=mesh,
        in_specs=(
            P("ep", "tp", None),
            P("ep", "tp", None),
            P("ep", "tp", None),
            P("tp"),
            P(),
            P(),
            P("ep", None),
            P(),
            P("ep", None),
            P("ep", None),
            P("ep", None, "tp"),
            P("ep", None, "tp"),
            P("ep", "tp", None),
        ),
        out_specs=(P(("ep", "tp"), None), P(("ep", "tp"), None)),
        check_vma=False,
    )
```
